256 devices in a mesh: sp: 16 (over y, x), tp: 16 (over z, core).
Axes of the slice: x: 4, y: 4, z: 8, core: 2. Of those that a mesh axis runs over, the one named last changes fastest.
Arguments:
- tokens: bfloat16 [8192, 4096], P('sp', 'tp'), may hold values from -6 to 6
- pre_gain: float32 [2, 4096], replicated, may hold values from 0.1 to 1.9
- w_value: bfloat16 [2, 4096, 4096], P(None, 'sp', 'tp'), may hold values from -0.09375 to 0.09375
- w_gate: bfloat16 [2, 4096, 4096], P(None, 'sp', 'tp'), may hold values from -0.09375 to 0.09375
- conv_taps: float32 [2, 31, 4096], P(None, None, 'tp'), may hold values from -3.5 to 3.5
- conv_bias: float32 [2, 4096], P(None, 'tp'), may hold values from -3 to 3
- norm_gain: float32 [2, 4096], P(None, 'tp'), may hold values from 0.1 to 1.9
- norm_bias: float32 [2, 4096], P(None, 'tp'), may hold values from -3 to 3
- w_out: bfloat16 [2, 4096, 4096], P(None, 'sp', 'tp'), may hold values from -0.09375 to 0.09375
- post_gain: float32 [2, 4096], P(None, 'tp'), may hold values from 0.1 to 1.9
Outputs:
- stream: bfloat16 [8192, 4096], P('sp', 'tp')
The draws below stay inside these ranges and needn't reach their ends.
All inputs are finite; a program needn't handle non-finite values.
Results may differ from the reference program's by a relative error of at most 0.009.
Values may be sent and summed in bfloat16 or wider, within the bound.
No kernel may reach another device: no remote copies, remote signals or barrier semaphores. Data moves between devices by JAX's collectives and lax.ppermute only.
A program may use at most 64 MiB of HBM per device.

```python
import math
import jax
import jax.numpy as jnp
from jax import lax

D = 4096
CH = 4096
TAPS = 31
LAYERS = 2
TOKENS = 8192


def draw_conv_taps(key, part):
    first_key, second_key, third_key = jax.random.split(key, 3)
    channel = jnp.arange(CH, dtype=jnp.float32)
    phase = jax.random.uniform(first_key, (LAYERS, 1, 1), jnp.float32, 0.0, 2.0 * math.pi)
    rough = jax.random.uniform(second_key, (LAYERS, 1, CH), jnp.float32, -0.35, 0.35)
    factor = jnp.exp(1.2 * jnp.sin(2.0 * math.pi * 3.0 * channel / CH + phase) + rough)
    base = jnp.clip(jax.random.normal(third_key, (LAYERS, TAPS, CH), jnp.float32), -4.0, 4.0)
    return base * factor / math.sqrt(TAPS)


def steps_of(own_key, shape, shards, smallest, high):
    def one(position, blocks):
        steps = jax.random.uniform(jax.random.fold_in(jax.random.fold_in(own_key, 6), position), (blocks,), jnp.float32, smallest / len(shards), high / len(shards))
        return jnp.repeat(jnp.exp(steps), shape[position] // blocks).reshape((-1,) + (1,) * (len(shape) - position - 1))

    level = one(*shards[0])
    for cut in shards[1:]:
        level = level * one(*cut)
    return level


def scatter_about(own_key, shape, width, limit, cuts=(), held_as=jnp.bfloat16):
    entries = width * jax.random.normal(own_key, shape, jnp.float32)
    if cuts:
        entries = entries * steps_of(own_key, shape, cuts, -0.22, 0.18)
    return jnp.clip(entries, -limit, limit).astype(held_as)


def setup_inputs(seed: int = 0) -> dict:
    keys = jax.random.split(jax.random.key(seed), 11)
    tokens = scatter_about(keys[0], (TOKENS, D), 1.0, 6.0, ((0, 16), (1, 16)))
    pre_gain = jnp.clip(1.0 + 0.18 * jax.random.normal(keys[1], (LAYERS, D), jnp.float32), 0.1, 1.9)
    w_value = scatter_about(keys[2], (LAYERS, D, CH), D ** -0.5, 0.09375, ((1, 16), (2, 16)))
    w_gate = scatter_about(keys[3], (LAYERS, D, CH), D ** -0.5, 0.09375, ((1, 16), (2, 16)))
    conv_taps = draw_conv_taps(jax.random.fold_in(keys[10], 71), 0)
    conv_bias = scatter_about(keys[5], (LAYERS, CH), 0.5, 3.0, ((1, 16),), jnp.float32)
    norm_gain = jnp.clip(1.0 + 0.18 * jax.random.normal(keys[6], (LAYERS, CH), jnp.float32), 0.1, 1.9)
    norm_bias = scatter_about(keys[7], (LAYERS, CH), 0.5, 3.0, ((1, 16),), jnp.float32)
    w_out = scatter_about(keys[8], (LAYERS, CH, D), CH ** -0.5, 0.09375, ((1, 16), (2, 16)))
    post_gain = jnp.clip(1.0 + 0.18 * jax.random.normal(keys[9], (LAYERS, D), jnp.float32), 0.1, 1.9)
    return dict(tokens=tokens, pre_gain=pre_gain, w_value=w_value, w_gate=w_gate, conv_taps=conv_taps, conv_bias=conv_bias, norm_gain=norm_gain, norm_bias=norm_bias, w_out=w_out, post_gain=post_gain)


def reference(tokens, pre_gain, w_value, w_gate, conv_taps, conv_bias, norm_gain, norm_bias, w_out, post_gain):
    stream = tokens
    for layer_index in range(LAYERS):
        full_rows = stream.astype(jnp.float32)
        scale_rows = lax.rsqrt(lax.optimization_barrier(jnp.mean(full_rows * full_rows, axis=-1, keepdims=True)) + 1e-06)
        normed = (full_rows * scale_rows * pre_gain[layer_index]).astype(jnp.bfloat16)
        value_proj = jnp.dot(normed, w_value[layer_index], preferred_element_type=jnp.float32)
        gate_proj = jnp.dot(normed, w_gate[layer_index], preferred_element_type=jnp.float32)
        glu_out = (value_proj * jax.nn.sigmoid(gate_proj)).astype(jnp.bfloat16)
        padded = jnp.concatenate([jnp.zeros((TAPS - 1, CH), jnp.bfloat16), glu_out], axis=0).astype(jnp.float32)
        filtered = jnp.zeros((TOKENS, CH), jnp.float32) + conv_bias[layer_index]
        for tap_index in range(TAPS):
            filtered = filtered + padded[tap_index:tap_index + TOKENS] * conv_taps[layer_index, tap_index]
        centre = lax.optimization_barrier(jnp.sum(filtered, axis=-1)) / CH
        spread = jnp.maximum(lax.optimization_barrier(jnp.sum(filtered * filtered, axis=-1)) / CH - centre * centre, 0.0)
        shaped = (filtered - centre[:, None]) * lax.rsqrt(spread + 1e-05)[:, None]
        mixed = jax.nn.silu(shaped * norm_gain[layer_index] + norm_bias[layer_index]).astype(jnp.bfloat16)
        branch_low = jnp.dot(mixed, w_out[layer_index], preferred_element_type=jnp.float32).astype(jnp.bfloat16)
        branch = lax.optimization_barrier(branch_low).astype(jnp.float32)
        total = lax.optimization_barrier(jnp.sum(branch * branch, axis=-1))
        rescale = lax.rsqrt(total / D + 1e-06)[:, None]
        stream = (stream.astype(jnp.float32) + branch * rescale * post_gain[layer_index]).astype(jnp.bfloat16)
    return stream
```

```python
import functools

import jax
import jax.numpy as jnp
from jax import lax
from jax.experimental import pallas as pl
from jax.experimental.pallas import tpu as pltpu
from jax.sharding import Mesh
from jax.sharding import PartitionSpec as P

BF = jnp.bfloat16
F32 = jnp.float32
AXES = ("y", "x", "z", "c")
NY, NX, NZ, NC = 4, 4, 8, 2
TAPS = 31
HALO = 32
ROWS = 256
COLS = 512
WIDTH = 4096


def pairs(target):
    def index(y, x, z, c):
        return ((y * NX + x) * NZ + z) * NC + c

    out = []
    for y in range(NY):
        for x in range(NX):
            for z in range(NZ):
                for c in range(NC):
                    to = target(y, x, z, c)
                    if to is not None:
                        out.append((index(y, x, z, c), index(*to)))
    return out


def along_z(y, x, z, c):
    return y, x, (z + (1 if c == 0 else -1)) % NZ, c


def to_partner(y, x, z, c):
    return y, x, z, 1 - c


def to_next_rows(y, x, z, c):
    if c == 0:
        return y, x, z, 1
    place = y * NX + x + 1
    if place == NY * NX:
        return None
    return place // NX, place % NX, z, 0


RING = pairs(along_z)
SWAP = pairs(to_partner)
NEXT = pairs(to_next_rows)


def permute(v, perm):
    return lax.ppermute(v, AXES, perm)


def gather_z(own):
    mine, other = own, permute(own, SWAP)
    blocks = [own]
    for step in range(4):
        mine = permute(mine, RING)
        blocks.append(mine)
        if step < 3:
            other = permute(other, RING)
            blocks.append(permute(other, SWAP))
    return blocks


def sigmoid(v):
    return 0.5 * (1.0 + jnp.tanh(0.5 * v))


def start_weights(w_hbm, w_vmem, sems, mats):
    copies = []
    for c in range(NC):
        for k, m in enumerate(mats):
            k = k * NC + c
            copy = pltpu.make_async_copy(w_hbm.at[:, c, m], w_vmem.at[k], sems.at[k])
            copy.start()
            copies.append((k, copy))
    return dict(copies)


def project_kernel(with_branch, zb_ref, *refs):
    s_refs = refs[:8]
    refs = refs[8:]
    if with_branch:
        b_refs, post_ref = refs[:8], refs[8]
        refs = refs[9:]
    gain_ref, w_hbm, out_ref = refs[:3]
    refs = refs[3:]
    if with_branch:
        stream_ref, refs = refs[0], refs[1:]
    x_ref, w_vmem, acc_ref, sems = refs
    copies = start_weights(w_hbm, w_vmem, sems, (0, 1))
    if with_branch:
        total = jnp.zeros((ROWS, 1), F32)
        for b_ref in b_refs:
            b = b_ref[...].astype(F32)
            total = total + jnp.sum(b * b, axis=-1, keepdims=True)
        rescale = lax.rsqrt(total / WIDTH + 1e-6)
    square = jnp.zeros((ROWS, 1), F32)
    for j in range(8):
        zb = zb_ref[j]
        s = s_refs[j][...].astype(F32)
        if with_branch:
            s = (s + b_refs[j][...].astype(F32) * rescale * post_ref[zb]).astype(BF)
            if j == 0:
                stream_ref[...] = s
            s = s.astype(F32)
        square = square + jnp.sum(s * s, axis=-1, keepdims=True)
        x_ref[:, pl.ds(pl.multiple_of(zb * COLS, COLS), COLS)] = (s * gain_ref[zb]).astype(BF)
    scale = lax.rsqrt(square / WIDTH + 1e-6)
    for c in range(NC):
        for m in range(2):
            k = m * NC + c
            copies[k].wait()
            acc = jnp.dot(x_ref[...], w_vmem[k].reshape(WIDTH, 256), preferred_element_type=F32)
            if m == 0:
                acc_ref[...] = acc * scale
            else:
                out_ref[:, c * 256 : (c + 1) * 256] = (acc_ref[...] * sigmoid(acc * scale)).astype(BF)


def vmem():
    return pl.BlockSpec(memory_space=pltpu.VMEM)


def project(zb, s_blocks, gain, weights, b_blocks=None, post=None):
    with_branch = b_blocks is not None
    operands = [zb, *s_blocks]
    specs = [pl.BlockSpec(memory_space=pltpu.SMEM)] + [vmem()] * 8
    if with_branch:
        operands += [*b_blocks, post]
        specs += [vmem()] * 9
    operands += [gain, weights]
    specs += [vmem(), pl.BlockSpec(memory_space=pltpu.HBM)]
    shape = jax.ShapeDtypeStruct((ROWS, COLS), BF)
    return pl.pallas_call(
        functools.partial(project_kernel, with_branch),
        out_shape=(shape, shape) if with_branch else shape,
        in_specs=specs,
        out_specs=(vmem(), vmem()) if with_branch else vmem(),
        scratch_shapes=[
            pltpu.VMEM((ROWS, WIDTH), BF),
            pltpu.VMEM((4, 16, 256, 256), BF),
            pltpu.VMEM((ROWS, 256), F32),
            pltpu.SemaphoreType.DMA((4,)),
        ],
        compiler_params=pltpu.CompilerParams(vmem_limit_bytes=50 * 1024 * 1024),
        cost_estimate=pl.CostEstimate(
            flops=2 * ROWS * WIDTH * 1024, bytes_accessed=12 * 1024 * 1024, transcendentals=ROWS * COLS
        ),
        name="project",
    )(*operands)


def conv_kernel(before_ref, glu_ref, taps_ref, out_ref, x_ref):
    x_ref[0:HALO, :] = before_ref[...].astype(F32)
    x_ref[HALO:, :] = glu_ref[...].astype(F32)
    part = 128
    for lane in range(0, COLS, 128):
        taps = taps_ref[:, lane : lane + 128]
        for row in range(0, ROWS, part):
            acc = jnp.zeros((part, 128), F32)
            for r in range(1, 9):
                xs = x_ref[row + r : row + r + part + 24, lane : lane + 128]
                for q in range(4):
                    j = r + 8 * q - (HALO - TAPS + 1)
                    if 0 <= j < TAPS:
                        acc = acc + xs[8 * q : 8 * q + part] * taps[j : j + 1]
            out_ref[row : row + part, lane : lane + 128] = acc.astype(BF)


def conv(before, glu, taps):
    return pl.pallas_call(
        conv_kernel,
        out_shape=jax.ShapeDtypeStruct((ROWS, COLS), BF),
        in_specs=[vmem()] * 3,
        out_specs=vmem(),
        scratch_shapes=[pltpu.VMEM((HALO + ROWS, COLS), F32)],
        compiler_params=pltpu.CompilerParams(vmem_limit_bytes=4 * 1024 * 1024),
        cost_estimate=pl.CostEstimate(
            flops=2 * TAPS * ROWS * COLS, bytes_accessed=4 * ROWS * COLS, transcendentals=0
        ),
        name="conv",
    )(before, glu, taps)


def mix_kernel(last, zb_ref, *refs):
    u_refs = refs[:8]
    par_ref, w_hbm, out_ref = refs[8:11]
    refs = refs[11:]
    if last:
        square_ref, refs = refs[0], refs[1:]
    x_ref, w_vmem, sems = refs
    copies = start_weights(w_hbm, w_vmem, sems, (2,))
    total = jnp.zeros((ROWS, 1), F32)
    square = jnp.zeros((ROWS, 1), F32)
    for j in range(8):
        f = u_refs[j][...].astype(F32) + par_ref[zb_ref[j], 0:1]
        total = total + jnp.sum(f, axis=-1, keepdims=True)
        square = square + jnp.sum(f * f, axis=-1, keepdims=True)
    centre = total / WIDTH
    spread = jnp.maximum(square / WIDTH - centre * centre, 0.0)
    inverse = lax.rsqrt(spread + 1e-5)
    for j in range(8):
        zb = zb_ref[j]
        f = u_refs[j][...].astype(F32) + par_ref[zb, 0:1]
        v = (f - centre) * inverse * par_ref[zb, 1:2] + par_ref[zb, 2:3]
        x_ref[:, pl.ds(pl.multiple_of(zb * COLS, COLS), COLS)] = (v * sigmoid(v)).astype(BF)
    sums = jnp.zeros((ROWS, 1), F32)
    for c in range(NC):
        copies[c].wait()
        acc = jnp.dot(x_ref[...], w_vmem[c].reshape(WIDTH, 256), preferred_element_type=F32)
        branch = acc.astype(BF)
        out_ref[:, c * 256 : (c + 1) * 256] = branch
        if last:
            b = branch.astype(F32)
            sums = sums + jnp.sum(b * b, axis=-1, keepdims=True)
    if last:
        square_ref[...] = sums


def mix(zb, u_blocks, par, weights, last):
    shape = jax.ShapeDtypeStruct((ROWS, COLS), BF)
    return pl.pallas_call(
        functools.partial(mix_kernel, last),
        out_shape=(shape, jax.ShapeDtypeStruct((ROWS, 1), F32)) if last else shape,
        in_specs=[pl.BlockSpec(memory_space=pltpu.SMEM)] + [vmem()] * 9 + [pl.BlockSpec(memory_space=pltpu.HBM)],
        out_specs=(vmem(), vmem()) if last else vmem(),
        scratch_shapes=[
            pltpu.VMEM((ROWS, WIDTH), BF),
            pltpu.VMEM((2, 16, 256, 256), BF),
            pltpu.SemaphoreType.DMA((2,)),
        ],
        compiler_params=pltpu.CompilerParams(vmem_limit_bytes=50 * 1024 * 1024),
        cost_estimate=pl.CostEstimate(
            flops=2 * ROWS * WIDTH * COLS, bytes_accessed=8 * 1024 * 1024, transcendentals=ROWS * WIDTH
        ),
        name="mix",
    )(zb, *u_blocks, par, weights)


def gather_weights(w):
    out = lax.all_gather(w[None], ("y", "x", "c"), axis=0, tiled=True)
    return out.reshape(16, NC, *w.shape)


def halves(v, core):
    own = jnp.where(core == 0, v[:ROWS], v[ROWS:])
    other = jnp.where(core == 0, v[ROWS:], v[:ROWS])
    return own, other


def to_rows(v, core):
    own, other = halves(v, core)
    got = permute(other, SWAP)
    return jnp.where(core == 0, jnp.concatenate([own, got], 1), jnp.concatenate([got, own], 1))


def to_columns(v, core):
    half = v.shape[1] // 2
    own = jnp.where(core == 0, v[:, :half], v[:, half:])
    other = jnp.where(core == 0, v[:, half:], v[:, :half])
    got = permute(other, SWAP)
    return jnp.where(core == 0, jnp.concatenate([own, got], 0), jnp.concatenate([got, own], 0))


def pair_columns(v, core):
    got = permute(v, SWAP)
    return jnp.where(core == 0, jnp.concatenate([v, got], 1), jnp.concatenate([got, v], 1))


def shards(
    tokens, pre_gain, w_value, w_gate, conv_taps, conv_bias, norm_gain, norm_bias, w_out, post_gain
):
    z, core = lax.axis_index("z"), lax.axis_index("c")
    sign = jnp.where(core == 0, 1, -1)
    steps = jnp.array([0, -1, 1, -2, 2, -3, 3, -4], jnp.int32)
    zb = jnp.mod(z + sign * steps, NZ).astype(jnp.int32)

    weights = [gather_weights(jnp.stack([w_value[l], w_gate[l], w_out[l]])) for l in range(2)]

    small = jnp.concatenate([conv_bias, norm_gain, norm_bias, post_gain], 0)
    small = lax.all_gather(small, ("z", "c"), axis=1, tiled=True)
    gains = pre_gain.reshape(2, NZ, 1, COLS)
    taps = pair_columns(conv_taps.reshape(2 * TAPS, 256), core).reshape(2, TAPS, COLS)

    s_blocks = gather_z(to_rows(tokens, core))
    zb, small = lax.optimization_barrier((zb, small))
    small = small.reshape(8, NZ, COLS)
    par = [jnp.stack([small[l], small[2 + l], small[4 + l]], 1) for l in range(2)]
    post = small[6].reshape(NZ, 1, COLS)
    glu = project(zb, s_blocks, gains[0], weights[0])
    before = permute(glu[ROWS - HALO :], NEXT)
    u_blocks = gather_z(conv(before, glu, taps[0]))
    branch = mix(zb, u_blocks, par[0], weights[0], False)
    b_blocks = gather_z(branch)

    glu, stream = project(zb, s_blocks, gains[1], weights[1], b_blocks, post)
    stream = to_columns(stream, core)
    before = permute(glu[ROWS - HALO :], NEXT)
    u_blocks = gather_z(conv(before, glu, taps[1]))
    branch, square = mix(zb, u_blocks, par[1], weights[1], True)

    square = square.reshape(1, ROWS)
    nothing = jnp.zeros_like(square)
    both = jnp.where(core == 0, jnp.concatenate([square, nothing], 1), jnp.concatenate([nothing, square], 1))
    peers = lax.all_to_all(
        jnp.broadcast_to(both.reshape(1, 2 * ROWS), (16, 2 * ROWS)), ("z", "c"), 0, 0, tiled=True
    )
    rescale = lax.rsqrt(peers.sum(axis=0) / WIDTH + 1e-6)[:, None]
    branch = to_columns(branch, core)
    return (stream.astype(F32) + branch.astype(F32) * rescale * post_gain[1]).astype(BF)


def solution(mesh):
    fine = Mesh(mesh.devices.reshape(NY, NX, NZ, NC), AXES)
    sp, tp = ("y", "x"), ("z", "c")
    in_specs = (
        P(sp, tp),
        P(),
        P(None, sp, tp),
        P(None, sp, tp),
        P(None, None, tp),
        P(None, tp),
        P(None, tp),
        P(None, tp),
        P(None, sp, tp),
        P(None, tp),
    )
    return jax.shard_map(shards, mesh=fine, in_specs=in_specs, out_specs=P(sp, tp), check_vma=False)
```

```python
import functools

import jax
import jax.numpy as jnp
from jax import lax
from jax.experimental import pallas as pl
from jax.experimental.pallas import tpu as pltpu
from jax.sharding import Mesh
from jax.sharding import PartitionSpec as P

BF = jnp.bfloat16
F32 = jnp.float32
AXES = ("y", "x", "z", "c")
NY, NX, NZ, NC = 4, 4, 8, 2
TAPS = 31
HALO = 32
ROWS = 256
COLS = 512
WIDTH = 4096


def pairs(target):
    def index(y, x, z, c):
        return ((y * NX + x) * NZ + z) * NC + c

    out = []
    for y in range(NY):
        for x in range(NX):
            for z in range(NZ):
                for c in range(NC):
                    to = target(y, x, z, c)
                    if to is not None:
                        out.append((index(y, x, z, c), index(*to)))
    return out


def along_z(y, x, z, c):
    return y, x, (z + (1 if c == 0 else -1)) % NZ, c


def to_partner(y, x, z, c):
    return y, x, z, 1 - c


def to_next_rows(y, x, z, c):
    if c == 0:
        return y, x, z, 1
    place = y * NX + x + 1
    if place == NY * NX:
        return None
    return place // NX, place % NX, z, 0


RING = pairs(along_z)
SWAP = pairs(to_partner)
NEXT = pairs(to_next_rows)


def permute(v, perm):
    return lax.ppermute(v, AXES, perm)


def gather_z(own, side=None, due=0):
    mine, other = own, permute(own, SWAP)
    blocks = [own]
    for step in range(4):
        if side is not None and step == due:
            mine, side = lax.optimization_barrier((mine, side))
        mine = permute(mine, RING)
        blocks.append(mine)
        if step < 3:
            other = permute(other, RING)
            blocks.append(permute(other, SWAP))
    return blocks if side is None else (blocks, side)


def sigmoid(v):
    return 0.5 * (1.0 + jnp.tanh(0.5 * v))


def start_weights(w_hbm, w_vmem, sems, mats):
    copies = []
    for c in range(NC):
        for k, m in enumerate(mats):
            k = k * NC + c
            copy = pltpu.make_async_copy(w_hbm.at[:, c, m], w_vmem.at[k], sems.at[k])
            copy.start()
            copies.append((k, copy))
    return dict(copies)


def project_kernel(with_branch, zb_ref, *refs):
    s_refs = refs[:8]
    refs = refs[8:]
    if with_branch:
        b_refs, post_ref = refs[:8], refs[8]
        refs = refs[9:]
    gain_ref, refs = refs[0], refs[1:]
    if with_branch:
        *w_refs, out_ref, stream_ref, x_ref, acc_ref = refs
    else:
        w_hbm, out_ref, x_ref, w_vmem, acc_ref, sems = refs
        copies = start_weights(w_hbm, w_vmem, sems, (0, 1))
    if with_branch:
        total = jnp.zeros((ROWS, 1), F32)
        for b_ref in b_refs:
            b = b_ref[...].astype(F32)
            total = total + jnp.sum(b * b, axis=-1, keepdims=True)
        rescale = lax.rsqrt(total / WIDTH + 1e-6)
    square = jnp.zeros((ROWS, 1), F32)
    for j in range(8):
        zb = zb_ref[j]
        s = s_refs[j][...].astype(F32)
        if with_branch:
            s = (s + b_refs[j][...].astype(F32) * rescale * post_ref[zb]).astype(BF)
            if j == 0:
                stream_ref[...] = s
            s = s.astype(F32)
        square = square + jnp.sum(s * s, axis=-1, keepdims=True)
        x_ref[:, pl.ds(pl.multiple_of(zb * COLS, COLS), COLS)] = (s * gain_ref[zb]).astype(BF)
    scale = lax.rsqrt(square / WIDTH + 1e-6)
    if with_branch:
        for m in range(2):

            @pl.loop(0, NC)
            def _(c):
                lanes = pl.ds(pl.multiple_of(c * 256, 256), 256)
                acc = scale * jnp.dot(
                    x_ref[...], w_refs[m][:, c].reshape(WIDTH, 256), preferred_element_type=F32
                )
                if m == 0:
                    acc_ref[:, lanes] = acc
                else:
                    out_ref[:, lanes] = (acc_ref[:, lanes] * sigmoid(acc)).astype(BF)

        return
    for c in range(NC):
        for m in range(2):
            k = m * NC + c
            copies[k].wait()
            acc = jnp.dot(x_ref[...], w_vmem[k].reshape(WIDTH, 256), preferred_element_type=F32)
            if m == 0:
                acc_ref[:, 0:256] = acc * scale
            else:
                out_ref[:, c * 256 : (c + 1) * 256] = (acc_ref[:, 0:256] * sigmoid(acc * scale)).astype(BF)


def vmem():
    return pl.BlockSpec(memory_space=pltpu.VMEM)


def project(zb, s_blocks, gain, weights, b_blocks=None, post=None):
    with_branch = b_blocks is not None
    operands = [zb, *s_blocks]
    specs = [pl.BlockSpec(memory_space=pltpu.SMEM)] + [vmem()] * 8
    if with_branch:
        operands += [*b_blocks, post]
        specs += [vmem()] * 9
    operands += [gain, *weights]
    specs += [vmem()] + ([vmem()] * 2 if with_branch else [pl.BlockSpec(memory_space=pltpu.HBM)])
    fetched = [] if with_branch else [pltpu.VMEM((4, 16, 256, 256), BF)]
    sems = [] if with_branch else [pltpu.SemaphoreType.DMA((4,))]
    shape = jax.ShapeDtypeStruct((ROWS, COLS), BF)
    return pl.pallas_call(
        functools.partial(project_kernel, with_branch),
        out_shape=(shape, shape) if with_branch else shape,
        in_specs=specs,
        out_specs=(vmem(), vmem()) if with_branch else vmem(),
        scratch_shapes=[
            pltpu.VMEM((ROWS, WIDTH), BF),
            *fetched,
            pltpu.VMEM((ROWS, COLS), F32),
            *sems,
        ],
        compiler_params=pltpu.CompilerParams(vmem_limit_bytes=(24 if with_branch else 50) * 1024 * 1024),
        cost_estimate=pl.CostEstimate(
            flops=2 * ROWS * WIDTH * 1024, bytes_accessed=12 * 1024 * 1024, transcendentals=ROWS * COLS
        ),
        name="project",
    )(*operands)


def conv_kernel(before_ref, glu_ref, taps_ref, out_ref, x_ref):
    x_ref[0:HALO, :] = before_ref[...].astype(F32)
    x_ref[HALO:, :] = glu_ref[...].astype(F32)
    part = 128

    @pl.loop(0, COLS // 128)
    def _(tile):
        lanes = pl.ds(pl.multiple_of(tile * 128, 128), 128)
        taps = taps_ref[:, lanes]
        for row in range(0, ROWS, part):
            acc = jnp.zeros((part, 128), F32)
            for r in range(1, 9):
                xs = x_ref[row + r : row + r + part + 24, lanes]
                for q in range(4):
                    j = r + 8 * q - (HALO - TAPS + 1)
                    if 0 <= j < TAPS:
                        acc = acc + xs[8 * q : 8 * q + part] * taps[j : j + 1]
            out_ref[row : row + part, lanes] = acc.astype(BF)


def conv(before, glu, taps):
    return pl.pallas_call(
        conv_kernel,
        out_shape=jax.ShapeDtypeStruct((ROWS, COLS), BF),
        in_specs=[vmem()] * 3,
        out_specs=vmem(),
        scratch_shapes=[pltpu.VMEM((HALO + ROWS, COLS), F32)],
        compiler_params=pltpu.CompilerParams(vmem_limit_bytes=4 * 1024 * 1024),
        cost_estimate=pl.CostEstimate(
            flops=2 * TAPS * ROWS * COLS, bytes_accessed=4 * ROWS * COLS, transcendentals=0
        ),
        name="conv",
    )(before, glu, taps)


def mix_kernel(last, zb_ref, *refs):
    u_refs = refs[:8]
    par_ref, w_ref, out_ref = refs[8:11]
    refs = refs[11:]
    if last:
        square_ref, refs = refs[0], refs[1:]
    (x_ref,) = refs
    total = jnp.zeros((ROWS, 1), F32)
    square = jnp.zeros((ROWS, 1), F32)
    for j in range(8):
        f = u_refs[j][...].astype(F32) + par_ref[zb_ref[j], 0:1]
        total = total + jnp.sum(f, axis=-1, keepdims=True)
        square = square + jnp.sum(f * f, axis=-1, keepdims=True)
    centre = total / WIDTH
    spread = jnp.maximum(square / WIDTH - centre * centre, 0.0)
    inverse = lax.rsqrt(spread + 1e-5)
    for j in range(8):
        zb = zb_ref[j]
        f = u_refs[j][...].astype(F32) + par_ref[zb, 0:1]
        v = (f - centre) * inverse * par_ref[zb, 1:2] + par_ref[zb, 2:3]
        x_ref[:, pl.ds(pl.multiple_of(zb * COLS, COLS), COLS)] = (v * sigmoid(v)).astype(BF)
    @pl.loop(0, NC, init_carry=jnp.zeros((ROWS, 1), F32))
    def sums(c, carry):
        acc = jnp.dot(x_ref[...], w_ref[:, c].reshape(WIDTH, 256), preferred_element_type=F32)
        branch = acc.astype(BF)
        out_ref[:, pl.ds(pl.multiple_of(c * 256, 256), 256)] = branch
        if not last:
            return carry
        b = branch.astype(F32)
        return carry + jnp.sum(b * b, axis=-1, keepdims=True)

    if last:
        square_ref[...] = sums


def mix(zb, u_blocks, par, weights, last):
    shape = jax.ShapeDtypeStruct((ROWS, COLS), BF)
    return pl.pallas_call(
        functools.partial(mix_kernel, last),
        out_shape=(shape, jax.ShapeDtypeStruct((ROWS, 1), F32)) if last else shape,
        in_specs=[pl.BlockSpec(memory_space=pltpu.SMEM)] + [vmem()] * 10,
        out_specs=(vmem(), vmem()) if last else vmem(),
        scratch_shapes=[pltpu.VMEM((ROWS, WIDTH), BF)],
        compiler_params=pltpu.CompilerParams(vmem_limit_bytes=24 * 1024 * 1024),
        cost_estimate=pl.CostEstimate(
            flops=2 * ROWS * WIDTH * COLS, bytes_accessed=8 * 1024 * 1024, transcendentals=ROWS * WIDTH
        ),
        name="mix",
    )(zb, *u_blocks, par, weights)


def gather_weights(w):
    out = lax.all_gather(w[None], ("y", "x", "c"), axis=0, tiled=True)
    return out.reshape(16, NC, *w.shape)


def halves(v, core):
    own = jnp.where(core == 0, v[:ROWS], v[ROWS:])
    other = jnp.where(core == 0, v[ROWS:], v[:ROWS])
    return own, other


def to_rows(v, core):
    own, other = halves(v, core)
    got = permute(other, SWAP)
    return jnp.where(core == 0, jnp.concatenate([own, got], 1), jnp.concatenate([got, own], 1))


def to_columns(v, core):
    half = v.shape[1] // 2
    own = jnp.where(core == 0, v[:, :half], v[:, half:])
    other = jnp.where(core == 0, v[:, half:], v[:, :half])
    got = permute(other, SWAP)
    return jnp.where(core == 0, jnp.concatenate([own, got], 0), jnp.concatenate([got, own], 0))


def pair_columns(v, core):
    got = permute(v, SWAP)
    return jnp.where(core == 0, jnp.concatenate([v, got], 1), jnp.concatenate([got, v], 1))


def shards(
    tokens, pre_gain, w_value, w_gate, conv_taps, conv_bias, norm_gain, norm_bias, w_out, post_gain
):
    z, core = lax.axis_index("z"), lax.axis_index("c")
    sign = jnp.where(core == 0, 1, -1)
    steps = jnp.array([0, -1, 1, -2, 2, -3, 3, -4], jnp.int32)
    zb = jnp.mod(z + sign * steps, NZ).astype(jnp.int32)

    stacks = [jnp.stack([w_value[l], w_gate[l], w_out[l]]) for l in range(2)]
    weights = [gather_weights(stack) for stack in stacks]

    small = jnp.concatenate([conv_bias, norm_gain, norm_bias, post_gain], 0)
    small = lax.all_gather(small, ("z", "c"), axis=1, tiled=True)
    gains = pre_gain.reshape(2, NZ, 1, COLS)
    taps = pair_columns(conv_taps.reshape(2 * TAPS, 256), core).reshape(2, TAPS, COLS)

    s_blocks = gather_z(to_rows(tokens, core))
    zb, small = lax.optimization_barrier((zb, small))
    small = small.reshape(8, NZ, COLS)
    par = [jnp.stack([small[l], small[2 + l], small[4 + l]], 1) for l in range(2)]
    post = small[6].reshape(NZ, 1, COLS)
    glu = project(zb, s_blocks, gains[0], weights[:1])
    before = permute(glu[ROWS - HALO :], NEXT)
    glu, first = lax.optimization_barrier((glu, weights[0]))
    u_blocks, out0 = gather_z(conv(before, glu, taps[0]), first[:, :, 2], 2)
    branch = mix(zb, u_blocks, par[0], out0, False)
    b_blocks, second = gather_z(branch, (weights[1][:, :, 0], weights[1][:, :, 1]), 3)

    glu, stream = project(zb, s_blocks, gains[1], second, b_blocks, post)
    stream = to_columns(stream, core)
    before = permute(glu[ROWS - HALO :], NEXT)
    glu, last = lax.optimization_barrier((glu, weights[1]))
    u_blocks, out1 = gather_z(conv(before, glu, taps[1]), last[:, :, 2], 2)
    branch, square = mix(zb, u_blocks, par[1], out1, True)

    square = square.reshape(1, ROWS)
    nothing = jnp.zeros_like(square)
    both = jnp.where(core == 0, jnp.concatenate([square, nothing], 1), jnp.concatenate([nothing, square], 1))
    peers = lax.all_to_all(
        jnp.broadcast_to(both.reshape(1, 2 * ROWS), (16, 2 * ROWS)), ("z", "c"), 0, 0, tiled=True
    )
    rescale = lax.rsqrt(peers.sum(axis=0) / WIDTH + 1e-6)[:, None]
    branch = to_columns(branch, core)
    return (stream.astype(F32) + branch.astype(F32) * rescale * post_gain[1]).astype(BF)


def solution(mesh):
    fine = Mesh(mesh.devices.reshape(NY, NX, NZ, NC), AXES)
    sp, tp = ("y", "x"), ("z", "c")
    in_specs = (
        P(sp, tp),
        P(),
        P(None, sp, tp),
        P(None, sp, tp),
        P(None, None, tp),
        P(None, tp),
        P(None, tp),
        P(None, tp),
        P(None, sp, tp),
        P(None, tp),
    )
    return jax.shard_map(shards, mesh=fine, in_specs=in_specs, out_specs=P(sp, tp), check_vma=False)
```

```python
import functools

import jax
import jax.numpy as jnp
from jax import lax
from jax.experimental import pallas as pl
from jax.experimental.pallas import tpu as pltpu
from jax.sharding import Mesh
from jax.sharding import PartitionSpec as P


BF = jnp.bfloat16
F32 = jnp.float32
AXES = ("y", "x", "z", "c")
NY, NX, NZ, NC = 4, 4, 8, 2
TAPS = 31
HALO = 32
ROWS = 256
COLS = 512
WIDTH = 4096


def pairs(target):
    def index(y, x, z, c):
        return ((y * NX + x) * NZ + z) * NC + c

    out = []
    for y in range(NY):
        for x in range(NX):
            for z in range(NZ):
                for c in range(NC):
                    to = target(y, x, z, c)
                    if to is not None:
                        out.append((index(y, x, z, c), index(*to)))
    return out


def along_z(y, x, z, c):
    return y, x, (z + (1 if c == 0 else -1)) % NZ, c


def to_partner(y, x, z, c):
    return y, x, z, 1 - c


def to_next_rows(y, x, z, c):
    if c == 0:
        return y, x, z, 1
    place = y * NX + x + 1
    if place == NY * NX:
        return None
    return place // NX, place % NX, z, 0


RING = pairs(along_z)
SWAP = pairs(to_partner)
NEXT = pairs(to_next_rows)


def permute(v, perm):
    return lax.ppermute(v, AXES, perm)


def gather_z(own):
    mine, other = own, permute(own, SWAP)
    blocks = [own]
    for step in range(4):
        mine = permute(mine, RING)
        blocks.append(mine)
        if step < 3:
            other = permute(other, RING)
            blocks.append(permute(other, SWAP))
    return blocks


def sigmoid(v):
    return 0.5 * (1.0 + jnp.tanh(0.5 * v))


def start_weights(w_hbm, w_vmem, sems, mats):
    copies = []
    for c in range(NC):
        for k, m in enumerate(mats):
            k = k * NC + c
            copy = pltpu.make_async_copy(w_hbm.at[:, c, m], w_vmem.at[k], sems.at[k])
            copy.start()
            copies.append((k, copy))
    return dict(copies)


def project_kernel(with_branch, zb_ref, *refs):
    s_refs, refs = refs[:8], refs[8:]
    if with_branch:
        b_refs, post_ref, refs = refs[:8], refs[8], refs[9:]
    gain_ref, refs = refs[0], refs[1:]
    if with_branch:
        *w_refs, out_ref, stream_ref, x_ref, acc_ref = refs
    else:
        w_hbm, out_ref, x_ref, w_vmem, acc_ref, sems = refs
        copies = start_weights(w_hbm, w_vmem, sems, (0, 1))
    if with_branch:
        total = jnp.zeros((ROWS, 1), F32)
        for b_ref in b_refs:
            b = b_ref[...].astype(F32)
            total = total + jnp.sum(b * b, axis=-1, keepdims=True)
        rescale = lax.rsqrt(total / WIDTH + 1e-6)
    square = jnp.zeros((ROWS, 1), F32)
    for j in range(8):
        zb = zb_ref[j]
        s = s_refs[j][...].astype(F32)
        if with_branch:
            s = (s + b_refs[j][...].astype(F32) * rescale * post_ref[zb]).astype(BF)
            if j == 0:
                stream_ref[...] = s
            s = s.astype(F32)
        square = square + jnp.sum(s * s, axis=-1, keepdims=True)
        x_ref[:, pl.ds(pl.multiple_of(zb * COLS, COLS), COLS)] = (s * gain_ref[zb]).astype(BF)
    scale = lax.rsqrt(square / WIDTH + 1e-6)
    if with_branch:
        for m in range(2):

            @pl.loop(0, NC)
            def _(c):
                lanes = pl.ds(pl.multiple_of(c * 256, 256), 256)
                acc = scale * jnp.dot(
                    x_ref[...], w_refs[m][:, c].reshape(WIDTH, 256), preferred_element_type=F32
                )
                if m == 0:
                    acc_ref[:, lanes] = acc
                else:
                    out_ref[:, lanes] = (acc_ref[:, lanes] * sigmoid(acc)).astype(BF)

        return
    for c in range(NC):
        for m in range(2):
            k = m * NC + c
            copies[k].wait()
            acc = jnp.dot(x_ref[...], w_vmem[k].reshape(WIDTH, 256), preferred_element_type=F32)
            if m == 0:
                acc_ref[:, 0:256] = acc * scale
            else:
                out_ref[:, c * 256 : (c + 1) * 256] = (acc_ref[:, 0:256] * sigmoid(acc * scale)).astype(BF)


def vmem():
    return pl.BlockSpec(memory_space=pltpu.VMEM)


def project(zb, s_blocks, gain, weights, b_blocks=None, post=None):
    with_branch = b_blocks is not None
    operands = [zb, *s_blocks]
    specs = [pl.BlockSpec(memory_space=pltpu.SMEM)] + [vmem()] * len(s_blocks)
    if with_branch:
        operands += [*b_blocks, post]
        specs += [vmem()] * (len(b_blocks) + 1)
    operands += [gain, *weights]
    specs += [vmem()] + ([vmem()] * 2 if with_branch else [pl.BlockSpec(memory_space=pltpu.HBM)])
    fetched = [] if with_branch else [pltpu.VMEM((4, 16, 256, 256), BF)]
    sems = [] if with_branch else [pltpu.SemaphoreType.DMA((4,))]
    shape = jax.ShapeDtypeStruct((ROWS, COLS), BF)
    return pl.pallas_call(
        functools.partial(project_kernel, with_branch),
        out_shape=(shape, shape) if with_branch else shape,
        in_specs=specs,
        out_specs=(vmem(), vmem()) if with_branch else vmem(),
        scratch_shapes=[
            pltpu.VMEM((ROWS, WIDTH), BF),
            *fetched,
            pltpu.VMEM((ROWS, COLS), F32),
            *sems,
        ],
        compiler_params=pltpu.CompilerParams(vmem_limit_bytes=(24 if with_branch else 50) * 1024 * 1024),
        cost_estimate=pl.CostEstimate(
            flops=2 * ROWS * WIDTH * 1024, bytes_accessed=12 * 1024 * 1024, transcendentals=ROWS * COLS
        ),
        name="project",
    )(*operands)


def conv_kernel(before_ref, glu_ref, taps_ref, out_ref, x_ref):
    x_ref[0:HALO, :] = before_ref[...].astype(F32)
    x_ref[HALO:, :] = glu_ref[...].astype(F32)
    part = 128
    for lane in range(0, COLS, 128):
        taps = taps_ref[:, lane : lane + 128]
        for row in range(0, ROWS, part):
            acc = jnp.zeros((part, 128), F32)
            for r in range(1, 9):
                xs = x_ref[row + r : row + r + part + 24, lane : lane + 128]
                for q in range(4):
                    j = r + 8 * q - (HALO - TAPS + 1)
                    if 0 <= j < TAPS:
                        acc = acc + xs[8 * q : 8 * q + part] * taps[j : j + 1]
            out_ref[row : row + part, lane : lane + 128] = acc.astype(BF)


def conv(before, glu, taps):
    return pl.pallas_call(
        conv_kernel,
        out_shape=jax.ShapeDtypeStruct((ROWS, COLS), BF),
        in_specs=[vmem()] * 3,
        out_specs=vmem(),
        scratch_shapes=[pltpu.VMEM((HALO + ROWS, COLS), F32)],
        compiler_params=pltpu.CompilerParams(vmem_limit_bytes=4 * 1024 * 1024),
        cost_estimate=pl.CostEstimate(
            flops=2 * TAPS * ROWS * COLS, bytes_accessed=4 * ROWS * COLS, transcendentals=0
        ),
        name="conv",
    )(before, glu, taps)


def mix_kernel(last, zb_ref, *refs):
    u_refs, refs = refs[:8], refs[8:]
    par_ref, w_ref, out_ref = refs[:3]
    refs = refs[3:]
    if last:
        square_ref, refs = refs[0], refs[1:]
    (x_ref,) = refs
    total = jnp.zeros((ROWS, 1), F32)
    square = jnp.zeros((ROWS, 1), F32)
    for j in range(8):
        f = u_refs[j][...].astype(F32) + par_ref[zb_ref[j], 0:1]
        total = total + jnp.sum(f, axis=-1, keepdims=True)
        square = square + jnp.sum(f * f, axis=-1, keepdims=True)
    centre = total / WIDTH
    spread = jnp.maximum(square / WIDTH - centre * centre, 0.0)
    inverse = lax.rsqrt(spread + 1e-5)
    for j in range(8):
        zb = zb_ref[j]
        f = u_refs[j][...].astype(F32) + par_ref[zb, 0:1]
        v = (f - centre) * inverse * par_ref[zb, 1:2] + par_ref[zb, 2:3]
        x_ref[:, pl.ds(pl.multiple_of(zb * COLS, COLS), COLS)] = (v * sigmoid(v)).astype(BF)

    @pl.loop(0, NC, init_carry=jnp.zeros((ROWS, 1), F32))
    def sums(c, carry):
        acc = jnp.dot(x_ref[...], w_ref[:, c].reshape(WIDTH, 256), preferred_element_type=F32)
        branch = acc.astype(BF)
        out_ref[:, pl.ds(pl.multiple_of(c * 256, 256), 256)] = branch
        if not last:
            return carry
        b = branch.astype(F32)
        return carry + jnp.sum(b * b, axis=-1, keepdims=True)

    if last:
        square_ref[...] = sums


def mix(zb, u_blocks, par, weights, last):
    shape = jax.ShapeDtypeStruct((ROWS, COLS), BF)
    return pl.pallas_call(
        functools.partial(mix_kernel, last),
        out_shape=(shape, jax.ShapeDtypeStruct((ROWS, 1), F32)) if last else shape,
        in_specs=[pl.BlockSpec(memory_space=pltpu.SMEM)] + [vmem()] * (len(u_blocks) + 2),
        out_specs=(vmem(), vmem()) if last else vmem(),
        scratch_shapes=[pltpu.VMEM((ROWS, WIDTH), BF)],
        compiler_params=pltpu.CompilerParams(vmem_limit_bytes=24 * 1024 * 1024),
        cost_estimate=pl.CostEstimate(
            flops=2 * ROWS * WIDTH * COLS, bytes_accessed=8 * 1024 * 1024, transcendentals=ROWS * WIDTH
        ),
        name="mix",
    )(zb, *u_blocks, par, weights)


def gather_weights(w):
    out = lax.all_gather(w[None], ("y", "x", "c"), axis=0, tiled=True)
    return out.reshape(16, NC, *w.shape)


def halves(v, core):
    own = jnp.where(core == 0, v[:ROWS], v[ROWS:])
    other = jnp.where(core == 0, v[ROWS:], v[:ROWS])
    return own, other


def to_rows(v, core):
    own, other = halves(v, core)
    got = permute(other, SWAP)
    return jnp.where(core == 0, jnp.concatenate([own, got], 1), jnp.concatenate([got, own], 1))


def to_columns(v, core):
    half = v.shape[1] // 2
    own = jnp.where(core == 0, v[:, :half], v[:, half:])
    other = jnp.where(core == 0, v[:, half:], v[:, :half])
    got = permute(other, SWAP)
    return jnp.where(core == 0, jnp.concatenate([own, got], 0), jnp.concatenate([got, own], 0))


def pair_columns(v, core):
    got = permute(v, SWAP)
    return jnp.where(core == 0, jnp.concatenate([v, got], 1), jnp.concatenate([got, v], 1))


def shards(
    tokens, pre_gain, w_value, w_gate, conv_taps, conv_bias, norm_gain, norm_bias, w_out, post_gain
):
    z, core = lax.axis_index("z"), lax.axis_index("c")
    sign = jnp.where(core == 0, 1, -1)
    steps = jnp.array([0, -1, 1, -2, 2, -3, 3, -4], jnp.int32)
    zb = jnp.mod(z + sign * steps, NZ).astype(jnp.int32)

    weights = [gather_weights(jnp.stack([w_value[l], w_gate[l], w_out[l]])) for l in range(2)]

    small = jnp.concatenate([conv_bias, norm_gain, norm_bias, post_gain], 0)
    small = lax.all_gather(small, ("z", "c"), axis=1, tiled=True)
    gains = pre_gain.reshape(2, NZ, 1, COLS)
    taps = pair_columns(conv_taps.reshape(2 * TAPS, 256), core).reshape(2, TAPS, COLS)

    s_blocks = gather_z(to_rows(tokens, core))
    zb, small = lax.optimization_barrier((zb, small))
    small = small.reshape(8, NZ, COLS)
    par = [jnp.stack([small[l], small[2 + l], small[4 + l]], 1) for l in range(2)]
    post = small[6].reshape(NZ, 1, COLS)
    glu = project(zb, s_blocks, gains[0], weights[:1])
    before = permute(glu[ROWS - HALO :], NEXT)
    glu, first = lax.optimization_barrier((glu, weights[0]))
    u_blocks = gather_z(conv(before, glu, taps[0]))
    out0 = first[:, :, 2]
    branch = mix(zb, u_blocks, par[0], out0, False)
    b_blocks = gather_z(branch)
    second = (weights[1][:, :, 0], weights[1][:, :, 1])

    glu, stream = project(zb, s_blocks, gains[1], second, b_blocks, post)
    stream = to_columns(stream, core)
    before = permute(glu[ROWS - HALO :], NEXT)
    glu, last = lax.optimization_barrier((glu, weights[1]))
    u_blocks = gather_z(conv(before, glu, taps[1]))
    out1 = last[:, :, 2]
    branch, square = mix(zb, u_blocks, par[1], out1, True)

    square = square.reshape(1, ROWS)
    nothing = jnp.zeros_like(square)
    both = jnp.where(core == 0, jnp.concatenate([square, nothing], 1), jnp.concatenate([nothing, square], 1))
    peers = lax.all_to_all(
        jnp.broadcast_to(both.reshape(1, 2 * ROWS), (16, 2 * ROWS)), ("z", "c"), 0, 0, tiled=True
    )
    rescale = lax.rsqrt(peers.sum(axis=0) / WIDTH + 1e-6)[:, None]
    branch = to_columns(branch, core)
    return (stream.astype(F32) + branch.astype(F32) * rescale * post_gain[1]).astype(BF)


def solution(mesh):
    fine = Mesh(mesh.devices.reshape(NY, NX, NZ, NC), AXES)
    sp, tp = ("y", "x"), ("z", "c")
    in_specs = (
        P(sp, tp),
        P(),
        P(None, sp, tp),
        P(None, sp, tp),
        P(None, None, tp),
        P(None, tp),
        P(None, tp),
        P(None, tp),
        P(None, sp, tp),
        P(None, tp),
    )

    return jax.shard_map(shards, mesh=fine, in_specs=in_specs, out_specs=P(sp, tp), check_vma=False)
```

```python
import functools

import jax
import jax.numpy as jnp
from jax import lax
from jax.experimental import pallas as pl
from jax.experimental.pallas import tpu as pltpu
from jax.sharding import Mesh
from jax.sharding import PartitionSpec as P


BF = jnp.bfloat16
F32 = jnp.float32
AXES = ("y", "x", "z", "c")
NY, NX, NZ, NC = 4, 4, 8, 2
TAPS = 31
HALO = 32
AHEAD = 3
ROWS = 256
COLS = 512
WIDTH = 4096


def pairs(target):
    def index(y, x, z, c):
        return ((y * NX + x) * NZ + z) * NC + c

    out = []
    for y in range(NY):
        for x in range(NX):
            for z in range(NZ):
                for c in range(NC):
                    to = target(y, x, z, c)
                    if to is not None:
                        out.append((index(y, x, z, c), index(*to)))
    return out


def along_z(y, x, z, c):
    return y, x, (z + (1 if c == 0 else -1)) % NZ, c


def to_partner(y, x, z, c):
    return y, x, z, 1 - c


def to_next_rows(y, x, z, c):
    if c == 0:
        return y, x, z, 1
    place = y * NX + x + 1
    if place == NY * NX:
        return None
    return place // NX, place % NX, z, 0


RING = pairs(along_z)
SWAP = pairs(to_partner)
NEXT = pairs(to_next_rows)


def permute(v, perm):
    return lax.ppermute(v, AXES, perm)


def gather_z(own):
    mine, other = own, permute(own, SWAP)
    blocks = [own]
    for step in range(4):
        mine = permute(mine, RING)
        blocks.append(mine)
        if step < 3:
            other = permute(other, RING)
            blocks.append(permute(other, SWAP))
    return blocks


def sigmoid(v):
    return 0.5 * (1.0 + jnp.tanh(0.5 * v))


def weight_copy(k, w_hbm, w_vmem, sems):
    c, m, h = k // 4, k // 2 % 2, k % 2
    return pltpu.make_async_copy(w_hbm.at[pl.ds(8 * h, 8), c, m], w_vmem.at[k], sems.at[k])


def project_kernel(with_branch, zb_ref, *refs):
    s_refs, refs = refs[:8], refs[8:]
    if with_branch:
        b_refs, post_ref, refs = refs[:8], refs[8], refs[9:]
    gain_ref, refs = refs[0], refs[1:]
    if with_branch:
        *w_refs, out_ref, stream_ref, x_ref, acc_ref = refs
    else:
        w_hbm, out_ref, x_ref, w_vmem, acc_ref, sems = refs
        for k in range(AHEAD):
            weight_copy(k, w_hbm, w_vmem, sems).start()
    if with_branch:
        total = jnp.zeros((ROWS, 1), F32)
        for b_ref in b_refs:
            b = b_ref[...].astype(F32)
            total = total + jnp.sum(b * b, axis=-1, keepdims=True)
        rescale = lax.rsqrt(total / WIDTH + 1e-6)
    square = jnp.zeros((ROWS, 1), F32)
    for j in range(8):
        zb = zb_ref[j]
        s = s_refs[j][...].astype(F32)
        if with_branch:
            s = (s + b_refs[j][...].astype(F32) * rescale * post_ref[zb]).astype(BF)
            if j == 0:
                stream_ref[...] = s
            s = s.astype(F32)
        square = square + jnp.sum(s * s, axis=-1, keepdims=True)
        x_ref[:, pl.ds(pl.multiple_of(zb * COLS, COLS), COLS)] = (s * gain_ref[zb]).astype(BF)
    scale = lax.rsqrt(square / WIDTH + 1e-6)
    if with_branch:
        for m in range(2):

            @pl.loop(0, NC)
            def _(c):
                lanes = pl.ds(pl.multiple_of(c * 256, 256), 256)
                acc = scale * jnp.dot(
                    x_ref[...], w_refs[m][:, c].reshape(WIDTH, 256), preferred_element_type=F32
                )
                if m == 0:
                    acc_ref[:, lanes] = acc
                else:
                    out_ref[:, lanes] = (acc_ref[:, lanes] * sigmoid(acc)).astype(BF)

        return
    acc_ref[...] = jnp.zeros_like(acc_ref)

    @pl.loop(0, 8)
    def _(k):
        weight_copy(k, w_hbm, w_vmem, sems).wait()

        @pl.when(k + AHEAD < 8)
        def _():
            weight_copy(k + AHEAD, w_hbm, w_vmem, sems).start()

        x = x_ref[:, pl.ds(pl.multiple_of(k % 2 * 2048, 2048), 2048)]
        acc_ref[k // 2] += jnp.dot(x, w_vmem[k].reshape(2048, 256), preferred_element_type=F32)

    for c in range(NC):
        value, gate = acc_ref[2 * c] * scale, acc_ref[2 * c + 1] * scale
        out_ref[:, c * 256 : (c + 1) * 256] = (value * sigmoid(gate)).astype(BF)


def vmem():
    return pl.BlockSpec(memory_space=pltpu.VMEM)


def project(zb, s_blocks, gain, weights, b_blocks=None, post=None):
    with_branch = b_blocks is not None
    operands = [zb, *s_blocks]
    specs = [pl.BlockSpec(memory_space=pltpu.SMEM)] + [vmem()] * len(s_blocks)
    if with_branch:
        operands += [*b_blocks, post]
        specs += [vmem()] * (len(b_blocks) + 1)
    operands += [gain, *weights]
    specs += [vmem()] + ([vmem()] * 2 if with_branch else [pl.BlockSpec(memory_space=pltpu.HBM)])
    fetched = [] if with_branch else [pltpu.VMEM((8, 8, 256, 256), BF)]
    sems = [] if with_branch else [pltpu.SemaphoreType.DMA((8,))]
    shape = jax.ShapeDtypeStruct((ROWS, COLS), BF)
    return pl.pallas_call(
        functools.partial(project_kernel, with_branch),
        out_shape=(shape, shape) if with_branch else shape,
        in_specs=specs,
        out_specs=(vmem(), vmem()) if with_branch else vmem(),
        scratch_shapes=[
            pltpu.VMEM((ROWS, WIDTH), BF),
            *fetched,
            pltpu.VMEM((ROWS, COLS) if with_branch else (4, ROWS, 256), F32),
            *sems,
        ],
        compiler_params=pltpu.CompilerParams(vmem_limit_bytes=(24 if with_branch else 50) * 1024 * 1024),
        cost_estimate=pl.CostEstimate(
            flops=2 * ROWS * WIDTH * 1024, bytes_accessed=12 * 1024 * 1024, transcendentals=ROWS * COLS
        ),
        name="project",
    )(*operands)


def conv_kernel(before_ref, glu_ref, taps_ref, out_ref, x_ref):
    x_ref[0:HALO, :] = before_ref[...].astype(F32)
    x_ref[HALO:, :] = glu_ref[...].astype(F32)
    part = 128
    for lane in range(0, COLS, 128):
        taps = taps_ref[:, lane : lane + 128]
        for row in range(0, ROWS, part):
            acc = jnp.zeros((part, 128), F32)
            for r in range(1, 9):
                xs = x_ref[row + r : row + r + part + 24, lane : lane + 128]
                for q in range(4):
                    j = r + 8 * q - (HALO - TAPS + 1)
                    if 0 <= j < TAPS:
                        acc = acc + xs[8 * q : 8 * q + part] * taps[j : j + 1]
            out_ref[row : row + part, lane : lane + 128] = acc.astype(BF)


def conv(before, glu, taps):
    return pl.pallas_call(
        conv_kernel,
        out_shape=jax.ShapeDtypeStruct((ROWS, COLS), BF),
        in_specs=[vmem()] * 3,
        out_specs=vmem(),
        scratch_shapes=[pltpu.VMEM((HALO + ROWS, COLS), F32)],
        compiler_params=pltpu.CompilerParams(vmem_limit_bytes=4 * 1024 * 1024),
        cost_estimate=pl.CostEstimate(
            flops=2 * TAPS * ROWS * COLS, bytes_accessed=4 * ROWS * COLS, transcendentals=0
        ),
        name="conv",
    )(before, glu, taps)


def mix_kernel(last, zb_ref, *refs):
    u_refs, refs = refs[:8], refs[8:]
    par_ref, w_ref, out_ref = refs[:3]
    refs = refs[3:]
    if last:
        square_ref, refs = refs[0], refs[1:]
    (x_ref,) = refs
    total = jnp.zeros((ROWS, 1), F32)
    square = jnp.zeros((ROWS, 1), F32)
    for j in range(8):
        f = u_refs[j][...].astype(F32) + par_ref[zb_ref[j], 0:1]
        total = total + jnp.sum(f, axis=-1, keepdims=True)
        square = square + jnp.sum(f * f, axis=-1, keepdims=True)
    centre = total / WIDTH
    spread = jnp.maximum(square / WIDTH - centre * centre, 0.0)
    inverse = lax.rsqrt(spread + 1e-5)
    for j in range(8):
        zb = zb_ref[j]
        f = u_refs[j][...].astype(F32) + par_ref[zb, 0:1]
        h = (f - centre) * inverse * (0.5 * par_ref[zb, 1:2]) + 0.5 * par_ref[zb, 2:3]
        x_ref[:, pl.ds(pl.multiple_of(zb * COLS, COLS), COLS)] = (h + h * jnp.tanh(h)).astype(BF)

    @pl.loop(0, NC, init_carry=jnp.zeros((ROWS, 1), F32))
    def sums(c, carry):
        acc = jnp.dot(x_ref[...], w_ref[:, c].reshape(WIDTH, 256), preferred_element_type=F32)
        branch = acc.astype(BF)
        out_ref[:, pl.ds(pl.multiple_of(c * 256, 256), 256)] = branch
        if not last:
            return carry
        b = branch.astype(F32)
        return carry + jnp.sum(b * b, axis=-1, keepdims=True)

    if last:
        square_ref[...] = sums


def mix(zb, u_blocks, par, weights, last):
    shape = jax.ShapeDtypeStruct((ROWS, COLS), BF)
    return pl.pallas_call(
        functools.partial(mix_kernel, last),
        out_shape=(shape, jax.ShapeDtypeStruct((ROWS, 1), F32)) if last else shape,
        in_specs=[pl.BlockSpec(memory_space=pltpu.SMEM)] + [vmem()] * (len(u_blocks) + 2),
        out_specs=(vmem(), vmem()) if last else vmem(),
        scratch_shapes=[pltpu.VMEM((ROWS, WIDTH), BF)],
        compiler_params=pltpu.CompilerParams(vmem_limit_bytes=24 * 1024 * 1024),
        cost_estimate=pl.CostEstimate(
            flops=2 * ROWS * WIDTH * COLS, bytes_accessed=8 * 1024 * 1024, transcendentals=ROWS * WIDTH
        ),
        name="mix",
    )(zb, *u_blocks, par, weights)


def stack_kernel(layer, *refs):
    *w_refs, out_ref, held, arrived, left = refs
    arrivals = [pltpu.make_async_copy(w.at[layer], held.at[k], arrived.at[k]) for k, w in enumerate(w_refs)]
    leaving = [pltpu.make_async_copy(held.at[k], out_ref.at[k], left.at[k]) for k in range(len(w_refs))]
    for copy in arrivals:
        copy.start()
    for arrival, copy in zip(arrivals, leaving):
        arrival.wait()
        copy.start()
    for copy in leaving:
        copy.wait()


def gather_weights(layer, *weights):
    shape = (len(weights), *weights[0].shape[1:])
    stacked = pl.pallas_call(
        functools.partial(stack_kernel, layer),
        out_shape=jax.ShapeDtypeStruct(shape, BF),
        in_specs=[pl.BlockSpec(memory_space=pltpu.HBM)] * len(weights),
        out_specs=pl.BlockSpec(memory_space=pltpu.HBM),
        scratch_shapes=[
            pltpu.VMEM(shape, BF),
            pltpu.SemaphoreType.DMA(shape[:1]),
            pltpu.SemaphoreType.DMA(shape[:1]),
        ],
        compiler_params=pltpu.CompilerParams(vmem_limit_bytes=63_300_000),
        name="stack",
    )(*weights)
    out = lax.all_gather(stacked, ("y", "x", "c"), axis=0, tiled=True)
    return out.reshape(16, NC, *shape)


def halves(v, core):
    own = jnp.where(core == 0, v[:ROWS], v[ROWS:])
    other = jnp.where(core == 0, v[ROWS:], v[:ROWS])
    return own, other


def to_rows(v, core):
    own, other = halves(v, core)
    got = permute(other, SWAP)
    return jnp.where(core == 0, jnp.concatenate([own, got], 1), jnp.concatenate([got, own], 1))


def to_columns(v, core):
    half = v.shape[1] // 2
    own = jnp.where(core == 0, v[:, :half], v[:, half:])
    other = jnp.where(core == 0, v[:, half:], v[:, :half])
    got = permute(other, SWAP)
    return jnp.where(core == 0, jnp.concatenate([own, got], 0), jnp.concatenate([got, own], 0))


def pair_columns(v, core):
    got = permute(v, SWAP)
    return jnp.where(core == 0, jnp.concatenate([v, got], 1), jnp.concatenate([got, v], 1))


def shards(
    tokens, pre_gain, w_value, w_gate, conv_taps, conv_bias, norm_gain, norm_bias, w_out, post_gain
):
    z, core = lax.axis_index("z"), lax.axis_index("c")
    sign = jnp.where(core == 0, 1, -1)
    steps = jnp.array([0, -1, 1, -2, 2, -3, 3, -4], jnp.int32)
    zb = jnp.mod(z + sign * steps, NZ).astype(jnp.int32)

    weights = [gather_weights(layer, w_value, w_gate, w_out) for layer in range(2)]

    small = jnp.concatenate([conv_bias, norm_gain, norm_bias, post_gain], 0)
    small = lax.all_gather(small, ("z", "c"), axis=1, tiled=True)
    gains = pre_gain.reshape(2, NZ, 1, COLS)
    taps = pair_columns(conv_taps.reshape(2 * TAPS, 256), core).reshape(2, TAPS, COLS)

    s_blocks = gather_z(to_rows(tokens, core))
    zb, small = lax.optimization_barrier((zb, small))
    small = small.reshape(8, NZ, COLS)
    par = [jnp.stack([small[l], small[2 + l], small[4 + l]], 1) for l in range(2)]
    post = small[6].reshape(NZ, 1, COLS)
    glu = project(zb, s_blocks, gains[0], weights[:1])
    before = permute(glu[ROWS - HALO :], NEXT)
    glu, first = lax.optimization_barrier((glu, weights[0]))
    u_blocks = gather_z(conv(before, glu, taps[0]))
    out0 = first[:, :, 2]
    branch = mix(zb, u_blocks, par[0], out0, False)
    b_blocks = gather_z(branch)
    second = (weights[1][:, :, 0], weights[1][:, :, 1])

    glu, stream = project(zb, s_blocks, gains[1], second, b_blocks, post)
    stream = to_columns(stream, core)
    before = permute(glu[ROWS - HALO :], NEXT)
    glu, last = lax.optimization_barrier((glu, weights[1]))
    u_blocks = gather_z(conv(before, glu, taps[1]))
    out1 = last[:, :, 2]
    branch, square = mix(zb, u_blocks, par[1], out1, True)

    square = square.reshape(1, ROWS)
    nothing = jnp.zeros_like(square)
    both = jnp.where(core == 0, jnp.concatenate([square, nothing], 1), jnp.concatenate([nothing, square], 1))
    peers = lax.all_to_all(
        jnp.broadcast_to(both.reshape(1, 2 * ROWS), (16, 2 * ROWS)), ("z", "c"), 0, 0, tiled=True
    )
    rescale = lax.rsqrt(peers.sum(axis=0) / WIDTH + 1e-6)[:, None]
    branch = to_columns(branch, core)
    return (stream.astype(F32) + branch.astype(F32) * rescale * post_gain[1]).astype(BF)


def solution(mesh):
    fine = Mesh(mesh.devices.reshape(NY, NX, NZ, NC), AXES)
    sp, tp = ("y", "x"), ("z", "c")
    in_specs = (
        P(sp, tp),
        P(),
        P(None, sp, tp),
        P(None, sp, tp),
        P(None, None, tp),
        P(None, tp),
        P(None, tp),
        P(None, tp),
        P(None, sp, tp),
        P(None, tp),
    )

    return jax.shard_map(shards, mesh=fine, in_specs=in_specs, out_specs=P(sp, tp), check_vma=False)
```

```python
import functools

import jax
import jax.numpy as jnp
from jax import lax
from jax.experimental import pallas as pl
from jax.experimental.pallas import tpu as pltpu
from jax.sharding import Mesh
from jax.sharding import PartitionSpec as P


BF = jnp.bfloat16
F32 = jnp.float32
AXES = ("y", "x", "z", "c")
NY, NX, NZ, NC = 4, 4, 8, 2
TAPS = 31
HALO = 32
AHEAD = 3
ROWS = 256
COLS = 512
WIDTH = 4096


def pairs(target):
    def index(y, x, z, c):
        return ((y * NX + x) * NZ + z) * NC + c

    out = []
    for y in range(NY):
        for x in range(NX):
            for z in range(NZ):
                for c in range(NC):
                    to = target(y, x, z, c)
                    if to is not None:
                        out.append((index(y, x, z, c), index(*to)))
    return out


def along_z(y, x, z, c):
    return y, x, (z + (1 if c == 0 else -1)) % NZ, c


def to_partner(y, x, z, c):
    return y, x, z, 1 - c


def to_next_rows(y, x, z, c):
    if c == 0:
        return y, x, z, 1
    place = y * NX + x + 1
    if place == NY * NX:
        return None
    return place // NX, place % NX, z, 0


RING = pairs(along_z)
SWAP = pairs(to_partner)
NEXT = pairs(to_next_rows)


def permute(v, perm):
    return lax.ppermute(v, AXES, perm)


def gather_z(own):
    mine, other = own, permute(own, SWAP)
    blocks = [own]
    for step in range(4):
        mine = permute(mine, RING)
        blocks.append(mine)
        if step < 3:
            other = permute(other, RING)
            blocks.append(permute(other, SWAP))
    return blocks


def sigmoid(v):
    return 0.5 * (1.0 + jnp.tanh(0.5 * v))


def weight_copy(k, w_hbm, w_vmem, sems):
    c, m, h = k // 4, k // 2 % 2, k % 2
    return pltpu.make_async_copy(w_hbm.at[pl.ds(8 * h, 8), c, m], w_vmem.at[k], sems.at[k])


def project_kernel(with_branch, zb_ref, *refs):
    s_refs, refs = refs[:8], refs[8:]
    if with_branch:
        b_refs, post_ref, refs = refs[:8], refs[8], refs[9:]
    gain_ref, refs = refs[0], refs[1:]
    if with_branch:
        *w_refs, out_ref, stream_ref, x_ref, acc_ref = refs
    else:
        w_hbm, out_ref, x_ref, w_vmem, acc_ref, sems = refs
        for k in range(AHEAD):
            weight_copy(k, w_hbm, w_vmem, sems).start()
    if with_branch:
        total = jnp.zeros((ROWS, 1), F32)
        for b_ref in b_refs:
            b = b_ref[...].astype(F32)
            total = total + jnp.sum(b * b, axis=-1, keepdims=True)
        rescale = lax.rsqrt(total / WIDTH + 1e-6)
    square = jnp.zeros((ROWS, 1), F32)
    for j in range(8):
        zb = zb_ref[j]
        s = s_refs[j][...].astype(F32)
        if with_branch:
            s = (s + b_refs[j][...].astype(F32) * rescale * post_ref[zb]).astype(BF)
            if j == 0:
                stream_ref[...] = s
            s = s.astype(F32)
        square = square + jnp.sum(s * s, axis=-1, keepdims=True)
        x_ref[:, pl.ds(pl.multiple_of(zb * COLS, COLS), COLS)] = (s * gain_ref[zb]).astype(BF)
    scale = lax.rsqrt(square / WIDTH + 1e-6)
    if with_branch:
        for m in range(2):

            @pl.loop(0, NC)
            def _(c):
                lanes = pl.ds(pl.multiple_of(c * 256, 256), 256)
                acc = scale * jnp.dot(
                    x_ref[...], w_refs[m][:, c].reshape(WIDTH, 256), preferred_element_type=F32
                )
                if m == 0:
                    acc_ref[:, lanes] = acc
                else:
                    out_ref[:, lanes] = (acc_ref[:, lanes] * sigmoid(acc)).astype(BF)

        return
    acc_ref[...] = jnp.zeros_like(acc_ref)

    @pl.loop(0, 8)
    def _(k):
        weight_copy(k, w_hbm, w_vmem, sems).wait()

        @pl.when(k + AHEAD < 8)
        def _():
            weight_copy(k + AHEAD, w_hbm, w_vmem, sems).start()

        x = x_ref[:, pl.ds(pl.multiple_of(k % 2 * 2048, 2048), 2048)]
        acc_ref[k // 2] += jnp.dot(x, w_vmem[k].reshape(2048, 256), preferred_element_type=F32)

    for c in range(NC):
        value, gate = acc_ref[2 * c] * scale, acc_ref[2 * c + 1] * scale
        out_ref[:, c * 256 : (c + 1) * 256] = (value * sigmoid(gate)).astype(BF)


def vmem():
    return pl.BlockSpec(memory_space=pltpu.VMEM)


def project(zb, s_blocks, gain, weights, b_blocks=None, post=None):
    with_branch = b_blocks is not None
    operands = [zb, *s_blocks]
    specs = [pl.BlockSpec(memory_space=pltpu.SMEM)] + [vmem()] * len(s_blocks)
    if with_branch:
        operands += [*b_blocks, post]
        specs += [vmem()] * (len(b_blocks) + 1)
    operands += [gain, *weights]
    specs += [vmem()] + ([vmem()] * 2 if with_branch else [pl.BlockSpec(memory_space=pltpu.HBM)])
    fetched = [] if with_branch else [pltpu.VMEM((8, 8, 256, 256), BF)]
    sems = [] if with_branch else [pltpu.SemaphoreType.DMA((8,))]
    shape = jax.ShapeDtypeStruct((ROWS, COLS), BF)
    return pl.pallas_call(
        functools.partial(project_kernel, with_branch),
        out_shape=(shape, shape) if with_branch else shape,
        in_specs=specs,
        out_specs=(vmem(), vmem()) if with_branch else vmem(),
        scratch_shapes=[
            pltpu.VMEM((ROWS, WIDTH), BF),
            *fetched,
            pltpu.VMEM((ROWS, COLS) if with_branch else (4, ROWS, 256), F32),
            *sems,
        ],
        compiler_params=pltpu.CompilerParams(vmem_limit_bytes=(24 if with_branch else 50) * 1024 * 1024),
        cost_estimate=pl.CostEstimate(
            flops=2 * ROWS * WIDTH * 1024, bytes_accessed=12 * 1024 * 1024, transcendentals=ROWS * COLS
        ),
        name="project",
    )(*operands)


def conv_kernel(before_ref, glu_ref, taps_ref, out_ref, x_ref):
    x_ref[0:HALO, :] = before_ref[...].astype(F32)
    x_ref[HALO:, :] = glu_ref[...].astype(F32)
    part = 128
    for lane in range(0, COLS, 128):
        taps = taps_ref[:, lane : lane + 128]
        for row in range(0, ROWS, part):
            acc = jnp.zeros((part, 128), F32)
            for r in range(1, 9):
                xs = x_ref[row + r : row + r + part + 24, lane : lane + 128]
                for q in range(4):
                    j = r + 8 * q - (HALO - TAPS + 1)
                    if 0 <= j < TAPS:
                        acc = acc + xs[8 * q : 8 * q + part] * taps[j : j + 1]
            out_ref[row : row + part, lane : lane + 128] = acc.astype(BF)


def conv(before, glu, taps):
    return pl.pallas_call(
        conv_kernel,
        out_shape=jax.ShapeDtypeStruct((ROWS, COLS), BF),
        in_specs=[vmem()] * 3,
        out_specs=vmem(),
        scratch_shapes=[pltpu.VMEM((HALO + ROWS, COLS), F32)],
        compiler_params=pltpu.CompilerParams(vmem_limit_bytes=4 * 1024 * 1024),
        cost_estimate=pl.CostEstimate(
            flops=2 * TAPS * ROWS * COLS, bytes_accessed=4 * ROWS * COLS, transcendentals=0
        ),
        name="conv",
    )(before, glu, taps)


def sums_kernel(zb_ref, *refs):
    *u_refs, par_ref, total_ref, square_ref = refs
    total = jnp.zeros((ROWS, 1), F32)
    square = jnp.zeros((ROWS, 1), F32)
    for j, u_ref in enumerate(u_refs):
        f = u_ref[...].astype(F32) + par_ref[zb_ref[j], 0:1]
        total = total + jnp.sum(f, axis=-1, keepdims=True)
        square = square + jnp.sum(f * f, axis=-1, keepdims=True)
    total_ref[...] = total
    square_ref[...] = square


def sums(zb, u_blocks, par):
    shape = jax.ShapeDtypeStruct((ROWS, 1), F32)
    return pl.pallas_call(
        sums_kernel,
        out_shape=(shape, shape),
        in_specs=[pl.BlockSpec(memory_space=pltpu.SMEM)] + [vmem()] * (len(u_blocks) + 1),
        out_specs=(vmem(), vmem()),
        compiler_params=pltpu.CompilerParams(vmem_limit_bytes=8 * 1024 * 1024),
        cost_estimate=pl.CostEstimate(
            flops=4 * ROWS * WIDTH, bytes_accessed=2 * ROWS * WIDTH, transcendentals=0
        ),
        name="sums",
    )(zb, *u_blocks, par)


def mix_kernel(last, zb_ref, *refs):
    u_refs, refs = refs[:8], refs[8:]
    par_ref, total_ref, partial_ref, w_ref, out_ref = refs[:5]
    refs = refs[5:]
    if last:
        square_ref, refs = refs[0], refs[1:]
    (x_ref,) = refs
    total, square = total_ref[...], partial_ref[...]
    for j in range(6, 8):
        f = u_refs[j][...].astype(F32) + par_ref[zb_ref[j], 0:1]
        total = total + jnp.sum(f, axis=-1, keepdims=True)
        square = square + jnp.sum(f * f, axis=-1, keepdims=True)
    centre = total / WIDTH
    spread = jnp.maximum(square / WIDTH - centre * centre, 0.0)
    inverse = lax.rsqrt(spread + 1e-5)
    for j in range(8):
        zb = zb_ref[j]
        f = u_refs[j][...].astype(F32) + par_ref[zb, 0:1]
        h = (f - centre) * inverse * (0.5 * par_ref[zb, 1:2]) + 0.5 * par_ref[zb, 2:3]
        x_ref[:, pl.ds(pl.multiple_of(zb * COLS, COLS), COLS)] = (h + h * jnp.tanh(h)).astype(BF)

    @pl.loop(0, NC, init_carry=jnp.zeros((ROWS, 1), F32))
    def sums(c, carry):
        acc = jnp.dot(x_ref[...], w_ref[:, c].reshape(WIDTH, 256), preferred_element_type=F32)
        branch = acc.astype(BF)
        out_ref[:, pl.ds(pl.multiple_of(c * 256, 256), 256)] = branch
        if not last:
            return carry
        b = branch.astype(F32)
        return carry + jnp.sum(b * b, axis=-1, keepdims=True)

    if last:
        square_ref[...] = sums


def mix(zb, u_blocks, par, partial, weights, last):
    shape = jax.ShapeDtypeStruct((ROWS, COLS), BF)
    return pl.pallas_call(
        functools.partial(mix_kernel, last),
        out_shape=(shape, jax.ShapeDtypeStruct((ROWS, 1), F32)) if last else shape,
        in_specs=[pl.BlockSpec(memory_space=pltpu.SMEM)] + [vmem()] * (len(u_blocks) + 4),
        out_specs=(vmem(), vmem()) if last else vmem(),
        scratch_shapes=[pltpu.VMEM((ROWS, WIDTH), BF)],
        compiler_params=pltpu.CompilerParams(vmem_limit_bytes=24 * 1024 * 1024),
        cost_estimate=pl.CostEstimate(
            flops=2 * ROWS * WIDTH * COLS, bytes_accessed=8 * 1024 * 1024, transcendentals=ROWS * WIDTH
        ),
        name="mix",
    )(zb, *u_blocks, par, *partial, weights)


def stack_kernel(layer, *refs):
    *w_refs, out_ref, held, arrived, left = refs
    arrivals = [pltpu.make_async_copy(w.at[layer], held.at[k], arrived.at[k]) for k, w in enumerate(w_refs)]
    leaving = [pltpu.make_async_copy(held.at[k], out_ref.at[k], left.at[k]) for k in range(len(w_refs))]
    for copy in arrivals:
        copy.start()
    for arrival, copy in zip(arrivals, leaving):
        arrival.wait()
        copy.start()
    for copy in leaving:
        copy.wait()


def gather_weights(layer, *weights):
    shape = (len(weights), *weights[0].shape[1:])
    stacked = pl.pallas_call(
        functools.partial(stack_kernel, layer),
        out_shape=jax.ShapeDtypeStruct(shape, BF),
        in_specs=[pl.BlockSpec(memory_space=pltpu.HBM)] * len(weights),
        out_specs=pl.BlockSpec(memory_space=pltpu.HBM),
        scratch_shapes=[
            pltpu.VMEM(shape, BF),
            pltpu.SemaphoreType.DMA(shape[:1]),
            pltpu.SemaphoreType.DMA(shape[:1]),
        ],
        compiler_params=pltpu.CompilerParams(vmem_limit_bytes=63_300_000),
        name="stack",
    )(*weights)
    out = lax.all_gather(stacked, ("y", "x", "c"), axis=0, tiled=True)
    return out.reshape(16, NC, *shape)


def halves(v, core):
    own = jnp.where(core == 0, v[:ROWS], v[ROWS:])
    other = jnp.where(core == 0, v[ROWS:], v[:ROWS])
    return own, other


def to_rows(v, core):
    own, other = halves(v, core)
    got = permute(other, SWAP)
    return jnp.where(core == 0, jnp.concatenate([own, got], 1), jnp.concatenate([got, own], 1))


def to_columns(v, core):
    half = v.shape[1] // 2
    own = jnp.where(core == 0, v[:, :half], v[:, half:])
    other = jnp.where(core == 0, v[:, half:], v[:, :half])
    got = permute(other, SWAP)
    return jnp.where(core == 0, jnp.concatenate([own, got], 0), jnp.concatenate([got, own], 0))


def pair_columns(v, core):
    got = permute(v, SWAP)
    return jnp.where(core == 0, jnp.concatenate([v, got], 1), jnp.concatenate([got, v], 1))


def shards(
    tokens, pre_gain, w_value, w_gate, conv_taps, conv_bias, norm_gain, norm_bias, w_out, post_gain
):
    z, core = lax.axis_index("z"), lax.axis_index("c")
    sign = jnp.where(core == 0, 1, -1)
    steps = jnp.array([0, -1, 1, -2, 2, -3, 3, -4], jnp.int32)
    zb = jnp.mod(z + sign * steps, NZ).astype(jnp.int32)

    weights = [gather_weights(layer, w_value, w_gate, w_out) for layer in range(2)]

    small = jnp.concatenate([conv_bias, norm_gain, norm_bias, post_gain], 0)
    small = lax.all_gather(small, ("z", "c"), axis=1, tiled=True)
    gains = pre_gain.reshape(2, NZ, 1, COLS)
    taps = pair_columns(conv_taps.reshape(2 * TAPS, 256), core).reshape(2, TAPS, COLS)

    s_blocks = gather_z(to_rows(tokens, core))
    zb, small = lax.optimization_barrier((zb, small))
    small = small.reshape(8, NZ, COLS)
    par = [jnp.stack([small[l], small[2 + l], small[4 + l]], 1) for l in range(2)]
    post = small[6].reshape(NZ, 1, COLS)
    glu = project(zb, s_blocks, gains[0], weights[:1])
    before = permute(glu[ROWS - HALO :], NEXT)
    glu, first = lax.optimization_barrier((glu, weights[0]))
    u_blocks = gather_z(conv(before, glu, taps[0]))
    out0 = first[:, :, 2]
    partial = sums(zb, u_blocks[:6], par[0])
    branch = mix(zb, u_blocks, par[0], partial, out0, False)
    b_blocks = gather_z(branch)
    second = (weights[1][:, :, 0], weights[1][:, :, 1])

    glu, stream = project(zb, s_blocks, gains[1], second, b_blocks, post)
    stream = to_columns(stream, core)
    before = permute(glu[ROWS - HALO :], NEXT)
    glu, last = lax.optimization_barrier((glu, weights[1]))
    u_blocks = gather_z(conv(before, glu, taps[1]))
    out1 = last[:, :, 2]
    partial = sums(zb, u_blocks[:6], par[1])
    branch, square = mix(zb, u_blocks, par[1], partial, out1, True)

    square = square.reshape(1, ROWS)
    nothing = jnp.zeros_like(square)
    both = jnp.where(core == 0, jnp.concatenate([square, nothing], 1), jnp.concatenate([nothing, square], 1))
    peers = lax.all_to_all(
        jnp.broadcast_to(both.reshape(1, 2 * ROWS), (16, 2 * ROWS)), ("z", "c"), 0, 0, tiled=True
    )
    rescale = lax.rsqrt(peers.sum(axis=0) / WIDTH + 1e-6)[:, None]
    branch = to_columns(branch, core)
    return (stream.astype(F32) + branch.astype(F32) * rescale * post_gain[1]).astype(BF)


def solution(mesh):
    fine = Mesh(mesh.devices.reshape(NY, NX, NZ, NC), AXES)
    sp, tp = ("y", "x"), ("z", "c")
    in_specs = (
        P(sp, tp),
        P(),
        P(None, sp, tp),
        P(None, sp, tp),
        P(None, None, tp),
        P(None, tp),
        P(None, tp),
        P(None, tp),
        P(None, sp, tp),
        P(None, tp),
    )

    return jax.shard_map(shards, mesh=fine, in_specs=in_specs, out_specs=P(sp, tp), check_vma=False)
```
